32 devices in a mesh: pp: 4 (over y, x), tp: 8 (over z, core).
Axes of the slice: x: 2, y: 2, z: 4, core: 2. Of those that a mesh axis runs over, the one named last changes fastest.
Arguments:
- entry_stream_rows: bfloat16 [256, 2048], P('pp', 'tp'), may hold values from -21 to 21
- layer_rescale_factor: float32 [4, 2048], P('pp'), may hold values from 0.1 to 1.9
- probe_projection: bfloat16 [4, 2048, 2048], P('pp', 'tp'), may hold values from -0.125 to 0.125
- retention_projection: bfloat16 [4, 2048, 2048], P('pp', 'tp'), may hold values from -0.125 to 0.125
- candidate_projection: bfloat16 [4, 2048, 2048], P('pp', 'tp'), may hold values from -0.125 to 0.125
- emission_filter_matrix: bfloat16 [4, 2048, 2048], P('pp', 'tp'), may hold values from -0.125 to 0.125
- retention_minimum: float32 [4, 2048], P('pp', 'tp'), may hold values from 0.88 to 0.9921875
- decay_spike: float32 [4, 128, 32], P('pp', None, 'tp'), may hold values from -2.1 to 0
- per_group_scale: float32 [4, 64], P('pp'), may hold values from 0.1 to 1.9
Outputs:
- outputs: bfloat16 [256, 2048], P('pp', 'tp')
The draws below stay inside these ranges and needn't reach their ends.
All inputs are finite; a program needn't handle non-finite values.
Results may differ from the reference program's by a relative error of at most 0.03.
Values may be sent and summed in bfloat16 or wider, within the bound.
A program may use at most 64 MiB of HBM per device.

```python
import math
import jax
import jax.numpy as jnp
from jax import lax

HEADS = 32
HEAD = 64
D = 2048
SEG = 64
MB_TOK = 128
SECTIONS = 4
MICRO = 2


def draw_entry_stream_rows(key, part):
    first_key, second_key, third_key = jax.random.split(jax.random.fold_in(key, 11), 3)
    rows = MICRO * MB_TOK
    column = jnp.arange(D, dtype=jnp.float32) / D
    values = jnp.clip(jax.random.normal(first_key, (rows, D), jnp.float32), -4.0, 4.0)
    row_scale = jnp.exp(jax.random.uniform(second_key, (rows, 1), jnp.float32, math.log(0.5), math.log(2.0)))
    rising = 3.0 ** (column - 0.5)
    col_scale = rising[None, :] * jnp.exp(jax.random.uniform(third_key, (1, D), jnp.float32, -0.35, 0.35))
    return (values * row_scale * col_scale).astype(jnp.bfloat16)


def draw_retention_minimum(key, part):
    first_key, second_key, third_key = jax.random.split(jax.random.fold_in(key, 23), 3)
    slow_share = 0.5
    slow_heads = jax.random.uniform(first_key, (SECTIONS, HEADS, 1), jnp.float32) < slow_share
    slow_gap = jnp.exp(jax.random.uniform(second_key, (SECTIONS, HEADS, HEAD), jnp.float32, math.log(1.0 / MB_TOK), math.log(4.0 / MB_TOK)))
    fast_gap = jnp.exp(jax.random.uniform(third_key, (SECTIONS, HEADS, HEAD), jnp.float32, math.log(0.04), math.log(0.12)))
    gap_all = jnp.where(slow_heads, slow_gap, fast_gap)
    return (1.0 - gap_all).reshape(SECTIONS, D).astype(jnp.float32)


def draw_decay_spike(key, part):
    first_key, second_key = jax.random.split(jax.random.fold_in(key, 37), 2)
    where_at = jax.random.randint(first_key, (SECTIONS, 3, HEADS), 0, MB_TOK)
    strength = jnp.log(jax.random.uniform(second_key, (SECTIONS, 3, HEADS), jnp.float32, 0.5, 0.8))
    positions = jnp.arange(MB_TOK, dtype=jnp.int32)[None, :, None, None]
    hit_mask = where_at[:, None, :, :] == positions
    return jnp.sum(jnp.where(hit_mask, strength[:, None, :, :], 0.0), axis=2).astype(jnp.float32)


def steps_of(own_key, shape, cuts, least, top_value):
    gain, own = 1.0, jax.random.fold_in(own_key, 6)
    for dim, blocks in cuts:
        heights = jnp.exp(jax.random.uniform(jax.random.fold_in(own, dim), (blocks,), jnp.float32, least / len(cuts), top_value / len(cuts)))
        gain = gain * jnp.repeat(heights, shape[dim] // blocks).reshape([-1 if axis == dim else 1 for axis in range(len(shape))])
    return gain


def normal_values(key, extent, spread, bound, cuts=(), kind=jnp.bfloat16):
    array = jax.random.normal(key, extent, jnp.float32) * spread
    if len(cuts) > 0:
        array = steps_of(key, extent, cuts, -0.22, 0.18) * array
    return jnp.clip(array, min=-bound, max=bound).astype(kind)


def setup_inputs(seed: int = 0) -> dict:
    keys = jax.random.split(jax.random.key(seed), 10)
    entry_stream_rows = draw_entry_stream_rows(jax.random.fold_in(keys[9], 71), 0)
    layer_rescale_factor = jnp.clip(1.0 + 0.18 * jax.random.normal(keys[1], (SECTIONS, D), jnp.float32), 0.1, 1.9)
    probe_projection = normal_values(keys[2], (SECTIONS, D, D), D ** -0.5, 0.125, ((0, 4), (1, 8)))
    retention_projection = normal_values(keys[3], (SECTIONS, D, D), D ** -0.5, 0.125, ((0, 4), (1, 8)))
    candidate_projection = normal_values(keys[4], (SECTIONS, D, D), D ** -0.5, 0.125, ((0, 4), (1, 8)))
    emission_filter_matrix = normal_values(keys[5], (SECTIONS, D, D), D ** -0.5, 0.125, ((0, 4), (1, 8)))
    retention_minimum = draw_retention_minimum(jax.random.fold_in(keys[9], 71), 0)
    decay_spike = draw_decay_spike(jax.random.fold_in(keys[9], 71), 0)
    per_group_scale = jnp.clip(1.0 + 0.18 * jax.random.normal(keys[8], (SECTIONS, HEAD), jnp.float32), 0.1, 1.9)
    return dict(entry_stream_rows=entry_stream_rows, layer_rescale_factor=layer_rescale_factor, probe_projection=probe_projection, retention_projection=retention_projection, candidate_projection=candidate_projection, emission_filter_matrix=emission_filter_matrix, retention_minimum=retention_minimum, decay_spike=decay_spike, per_group_scale=per_group_scale)


EPSILON = 1e-06
HIGHEST = lax.Precision.HIGHEST

def segment_scan(queries, key_in, log_forget, values, memory):
    head_count = queries.shape[0]
    length = queries.shape[1]
    blocks_count = length // SEG

    def split_blocks(tensor):
        return tensor.reshape(head_count, blocks_count, SEG, tensor.shape[-1]).transpose(1, 0, 2, 3)
    lower_mask = jnp.tril(jnp.ones((SEG, SEG), dtype=bool))[None]

    def one_block(memory_in, pieces):
        block_query, block_key, block_forget, block_value = pieces
        running = jnp.cumsum(block_forget, axis=1)
        query_scaled = block_query * jnp.exp(running)
        key_scaled = block_key * jnp.exp(-running)
        scores = jnp.einsum('hid,hjd->hij', query_scaled, key_scaled, precision=HIGHEST)
        scores = jnp.where(lower_mask, scores, 0.0)
        mixed_out = jnp.einsum('hij,hjv->hiv', scores, block_value, precision=HIGHEST)
        mixed_out = mixed_out + jnp.einsum('hid,hdv->hiv', query_scaled, memory_in, precision=HIGHEST)
        ending = running[:, -1:, :]
        carried_in = jnp.einsum('hjd,hjv->hdv', block_key * jnp.exp(ending - running), block_value, precision=HIGHEST)
        memory_out = jnp.exp(ending[:, 0, :])[:, :, None] * memory_in + carried_in
        return (memory_out, mixed_out)
    memory, mixed_out = lax.scan(one_block, memory, (split_blocks(queries), split_blocks(key_in), split_blocks(log_forget), split_blocks(values)))
    return (mixed_out.transpose(1, 0, 2, 3).reshape(head_count, length, values.shape[-1]), memory)

def head_norm(mixed_out, channel_gain):
    return mixed_out * lax.rsqrt(lax.optimization_barrier(jnp.mean(mixed_out * mixed_out, axis=-1, keepdims=True)) + EPSILON) * channel_gain

def reference(entry_stream_rows, layer_rescale_factor, probe_projection, retention_projection, candidate_projection, emission_filter_matrix, retention_minimum, decay_spike, per_group_scale):
    stream = entry_stream_rows
    for layer_ordinal in range(SECTIONS):
        wide_stream = stream.astype(jnp.float32)
        scaled = (wide_stream * layer_rescale_factor[layer_ordinal][None, :]).astype(jnp.bfloat16)
        inverse = lax.rsqrt(lax.optimization_barrier(jnp.mean(wide_stream * wide_stream, axis=1, keepdims=True)) + EPSILON)

        def per_head(tensor):
            return tensor.reshape(MICRO, MB_TOK, HEADS, HEAD).transpose(0, 2, 1, 3)
        projected = []
        for matrix in (probe_projection, retention_projection, candidate_projection, emission_filter_matrix):
            product = jnp.dot(scaled, matrix[layer_ordinal].T, preferred_element_type=jnp.float32) * inverse
            projected.append(per_head(product))
        query_pre, forget_pre, input_pre, gate_pre = projected
        lower_edge = retention_minimum[layer_ordinal].reshape(1, HEADS, 1, HEAD)
        remaining_portion = decay_spike[layer_ordinal].T[None, :, :, None]
        log_forget = jnp.logaddexp(jnp.log(lower_edge), jnp.log1p(-lower_edge) + jax.nn.log_sigmoid(forget_pre)) + remaining_portion
        key_in = (1.0 - lower_edge) * jax.nn.sigmoid(-forget_pre)
        queries = jax.nn.silu(query_pre)

        def one_sequence(pieces):
            zero_state = jnp.zeros((HEADS, HEAD, HEAD), jnp.float32)
            mixed_seq, final_state = segment_scan(pieces[0], pieces[1], pieces[2], pieces[3], zero_state)
            return mixed_seq
        mixed_out = lax.map(one_sequence, (queries, key_in, log_forget, input_pre))
        branch = head_norm(mixed_out, per_group_scale[layer_ordinal]) * jax.nn.silu(gate_pre)
        branch = branch.transpose(0, 2, 1, 3).reshape(MICRO * MB_TOK, D)
        stream = (wide_stream + branch).astype(jnp.bfloat16)
    return stream
```

```python
import functools

import jax
import jax.numpy as jnp
from jax import lax
from jax.experimental import pallas as pl
from jax.experimental.pallas import tpu as pltpu
from jax.sharding import PartitionSpec as P

HEAD = 64
EPSILON = 1e-06
F32 = jnp.float32
BF16 = jnp.bfloat16
NT = (((1,), (1,)), ((), ()))
NN = (((1,), (0,)), ((), ()))
TN = (((0,), (0,)), ((), ()))


def mm(a, b, dims):
    return lax.dot_general(a, b, dims, preferred_element_type=F32)


def sigmoid(v):
    return 1.0 / (1.0 + jnp.exp(-v))


def kernel(
    stages,
    lanes_axis,
    x_ref,
    gain_ref,
    wq_ref,
    wf_ref,
    wi_ref,
    wg_ref,
    low_ref,
    spike_ref,
    scale_ref,
    out_ref,
    weights,
    buf,
    res,
    spikes,
    state,
    w_sem,
    in_send,
    local_sem,
    direct_sem,
    forward_sem,
    send_sem,
    forward_send,
    out_sem,
):
    rows, cols = x_ref.shape
    heads = cols // HEAD
    width = gain_ref.shape[1]
    chips = lanes_axis // 2
    chunks = stages
    stage = lax.axis_index("pp")
    lane = lax.axis_index("tp")
    core = lax.rem(lane, 2)
    z = lane // 2
    partner = z * 2 + (1 - core)

    loads = []
    for role, ref in enumerate((wq_ref, wf_ref, wi_ref, wg_ref)):
        load = pltpu.make_async_copy(
            ref.at[0], weights.at[pl.ds(role * cols, cols)], w_sem.at[role]
        )
        load.start()
        loads.append(load)

    def to_first(far):
        target = lax.rem(z + far, chips) * 2 + core
        return pltpu.make_async_remote_copy(
            src_ref=x_ref,
            dst_ref=buf.at[stage, core, z],
            send_sem=in_send.at[far],
            recv_sem=direct_sem.at[stage],
            device_id={"pp": 0, "tp": target},
            device_id_type=pl.DeviceIdType.MESH,
        )

    own_copy = pltpu.make_async_copy(x_ref, buf.at[stage, core, z], direct_sem.at[stage])
    for far in range(1, chips):
        to_first(far).start()

    @pl.when(stage != 0)
    def _():
        to_first(0).start()

    @pl.when(stage == 0)
    def _():
        own_copy.start()

    head_of_lane = lax.broadcasted_iota(jnp.int32, (rows, cols), 1) // HEAD
    for part in range(2):
        piece = spike_ref[0, :, part * rows : (part + 1) * rows].T
        wide = jnp.zeros((rows, cols), F32)
        for h in range(heads):
            wide = jnp.where(head_of_lane == h, piece[:, h : h + 1], wide)
        spikes[part] = wide

    tri_row = lax.broadcasted_iota(jnp.int32, (rows, rows), 0)
    tri_col = lax.broadcasted_iota(jnp.int32, (rows, rows), 1)
    tril = tri_row >= tri_col
    tril_ones = jnp.where(tril, 1.0, 0.0).astype(BF16)
    tall_row = lax.rem(lax.broadcasted_iota(jnp.int32, (heads * rows, rows), 0), rows)
    tall_col = lax.broadcasted_iota(jnp.int32, (heads * rows, rows), 1)
    tall_mask = tall_row >= tall_col
    sq_row = lax.broadcasted_iota(jnp.int32, (cols, cols), 0) // HEAD
    sq_col = lax.broadcasted_iota(jnp.int32, (cols, cols), 1) // HEAD
    same_head = sq_row == sq_col
    mean_ones = jnp.where(same_head, 1.0 / HEAD, 0.0).astype(BF16)
    gain = gain_ref[...]
    span = 1.0 - low_ref[...]
    out_gain = jnp.concatenate([scale_ref[...]] * heads, axis=1)

    for load in loads:
        load.wait()

    def whole_wait(c, which, sem):
        half = buf.at[c, which]
        pltpu.make_async_copy(half, half, sem).wait()

    def forward(c):
        half = buf.at[c, core]
        return pltpu.make_async_remote_copy(
            src_ref=half,
            dst_ref=half,
            send_sem=forward_send.at[c],
            recv_sem=forward_sem.at[c],
            device_id={"pp": stage, "tp": partner},
            device_id_type=pl.DeviceIdType.MESH,
        )

    def to_next(c, far):
        target = lax.rem(z + far, chips) * 2 + core
        return pltpu.make_async_remote_copy(
            src_ref=res.at[c],
            dst_ref=buf.at[c, core, z],
            send_sem=send_sem.at[c],
            recv_sem=direct_sem.at[c],
            device_id={"pp": lax.rem(stage + 1, stages), "tp": target},
            device_id_type=pl.DeviceIdType.MESH,
        )

    def to_out(c):
        return pltpu.make_async_remote_copy(
            src_ref=res.at[c],
            dst_ref=out_ref,
            send_sem=send_sem.at[c],
            recv_sem=out_sem,
            device_id={"pp": c, "tp": lane},
            device_id_type=pl.DeviceIdType.MESH,
        )

    def step(c, carry):
        whole_wait(c, core, direct_sem.at[c])
        forward(c).start()
        whole_wait(c, 1 - core, forward_sem.at[c])

        current = jnp.concatenate(
            [buf[c, k % 2, k // 2] for k in range(lanes_axis)], axis=1
        ).astype(F32)
        inverse = lax.rsqrt(
            jnp.sum(current * current, axis=1, keepdims=True) / width + EPSILON
        )
        scaled = (current * gain).astype(BF16)
        projected = mm(scaled, weights[...], NT) * inverse
        query_pre = projected[:, 0 * cols : 1 * cols]
        forget_pre = projected[:, 1 * cols : 2 * cols]
        values = projected[:, 2 * cols : 3 * cols].astype(BF16)
        gate_pre = projected[:, 3 * cols : 4 * cols]

        key_in = span * sigmoid(-forget_pre)
        log_forget = jnp.log(1.0 - key_in) + spikes[lax.rem(c, 2)]
        high = log_forget.astype(BF16)
        low = (log_forget - high.astype(F32)).astype(BF16)
        running = mm(tril_ones, high, NN) + mm(tril_ones, low, NN)
        ending = running[rows - 1 : rows, :]
        query_scaled = query_pre * sigmoid(query_pre) * jnp.exp(running)
        key_scaled = (key_in * jnp.exp(-running)).astype(BF16)
        key_end = (key_in * jnp.exp(ending - running)).astype(BF16)
        query_bf = query_scaled.astype(BF16)
        tall_query = jnp.concatenate(
            [jnp.where(head_of_lane == h, query_scaled, 0.0).astype(BF16) for h in range(heads)],
            axis=0,
        )
        scores = jnp.where(tall_mask, mm(tall_query, key_scaled, NT), 0.0).astype(BF16)
        tall_mixed = mm(scores, values, NN)
        memory = jnp.where(lax.rem(c, 2) == 0, 0.0, state[...])
        mixed = mm(query_bf, memory.astype(BF16), NT)
        inner = tall_mixed[0:rows]
        for h in range(1, heads):
            inner = jnp.where(head_of_lane == h, tall_mixed[h * rows : (h + 1) * rows], inner)
        mixed = mixed + inner
        mean_square = mm((mixed * mixed).astype(BF16), mean_ones, NN)
        branch = mixed * lax.rsqrt(mean_square + EPSILON) * out_gain
        branch = branch * (gate_pre * sigmoid(gate_pre))
        res[c] = (buf[c, core, z].astype(F32) + branch).astype(BF16)

        @pl.when(stage != stages - 1)
        def _():
            for far in range(chips):
                to_next(c, far).start()

        @pl.when((stage == stages - 1) & (c != stage))
        def _():
            to_out(c).start()

        @pl.when((stage == stages - 1) & (c == stage))
        def _():
            pltpu.make_async_copy(res.at[c], out_ref, out_sem).start()

        added = jnp.where(same_head, mm(values, key_end, TN), 0.0)
        state[...] = memory * jnp.exp(ending) + added
        return carry

    lax.fori_loop(0, chunks, step, 0)

    for far in range(1, chips):
        to_first(far).wait_send()

    @pl.when(stage != 0)
    def _():
        to_first(0).wait_send()

    def drain(c, carry):
        forward(c).wait_send()

        @pl.when(stage != stages - 1)
        def _():
            whole_wait(c, core, send_sem.at[c])

        @pl.when((stage == stages - 1) & (c != stage))
        def _():
            to_out(c).wait_send()

        return carry

    lax.fori_loop(0, chunks, drain, 0)
    pltpu.make_async_copy(out_ref, out_ref, out_sem).wait()


def solution(mesh):
    stages = mesh.shape["pp"]
    lanes_axis = mesh.shape["tp"]
    chips = lanes_axis // 2

    def step(x, gain, wq, wf, wi, wg, low, spike, scale):
        rows, cols = x.shape
        width = gain.shape[1]
        vmem = pl.BlockSpec(memory_space=pltpu.VMEM)
        hbm = pl.BlockSpec(memory_space=pl.ANY)
        dma = pltpu.SemaphoreType.DMA
        return pl.pallas_call(
            functools.partial(kernel, stages, lanes_axis),
            out_shape=jax.ShapeDtypeStruct((rows, cols), BF16),
            in_specs=[vmem, vmem, hbm, hbm, hbm, hbm, vmem, vmem, vmem],
            out_specs=vmem,
            scratch_shapes=[
                pltpu.VMEM((4 * cols, width), BF16),
                pltpu.VMEM((stages, 2, chips, rows, cols), BF16),
                pltpu.VMEM((stages, rows, cols), BF16),
                pltpu.VMEM((2, rows, cols), F32),
                pltpu.VMEM((cols, cols), F32),
                dma((4,)),
                dma((chips,)),
                dma,
                dma((stages,)),
                dma((stages,)),
                dma((stages,)),
                dma((stages,)),
                dma,
            ],
            compiler_params=pltpu.CompilerParams(
                has_side_effects=True, vmem_limit_bytes=67043328
            ),
        )(x, gain, wq, wf, wi, wg, low, spike.transpose(0, 2, 1), scale)

    in_specs = (
        P("pp", "tp"),
        P("pp", None),
        P("pp", "tp", None),
        P("pp", "tp", None),
        P("pp", "tp", None),
        P("pp", "tp", None),
        P("pp", "tp"),
        P("pp", None, "tp"),
        P("pp", None),
    )
    return jax.shard_map(
        step, mesh=mesh, in_specs=in_specs, out_specs=P("pp", "tp"), check_vma=False
    )
```

```python
import functools

import jax
import jax.numpy as jnp
from jax import lax
from jax.experimental import pallas as pl
from jax.experimental.pallas import tpu as pltpu
from jax.sharding import PartitionSpec as P

HEAD = 64
EPSILON = 1e-06
F32 = jnp.float32
BF16 = jnp.bfloat16
NT = (((1,), (1,)), ((), ()))
NN = (((1,), (0,)), ((), ()))
TN = (((0,), (0,)), ((), ()))


def mm(a, b, dims):
    return lax.dot_general(a, b, dims, preferred_element_type=F32)


def sigmoid(v):
    return 1.0 / (1.0 + jnp.exp(-v))


def signal_to(semaphore, stage, lane):
    pl.semaphore_signal(
        semaphore,
        inc=1,
        device_id={"pp": stage, "tp": lane},
        device_id_type=pl.DeviceIdType.MESH,
    )


def kernel(
    stages,
    lanes_axis,
    x_ref,
    gain_ref,
    wq_ref,
    wf_ref,
    wi_ref,
    wg_ref,
    low_ref,
    spike_ref,
    scale_ref,
    out_ref,
    weights,
    buf,
    res,
    spikes,
    state,
    w_sem,
    in_send,
    direct_sem,
    forward_sem,
    send_sem,
    forward_send,
    out_sem,
):
    rows, cols = x_ref.shape
    heads = cols // HEAD
    width = gain_ref.shape[1]
    chips = lanes_axis // 2
    chunks = stages
    stage = lax.axis_index("pp")
    lane = lax.axis_index("tp")
    core = lax.rem(lane, 2)
    z = lane // 2
    partner = z * 2 + (1 - core)

    loads = []
    for role, ref in enumerate((wq_ref, wf_ref, wi_ref, wg_ref)):
        load = pltpu.make_async_copy(
            ref.at[0], weights.at[pl.ds(role * cols, cols)], w_sem.at[role]
        )
        load.start()
        loads.append(load)

    barrier = pltpu.get_barrier_semaphore()
    for up in range(stages):
        for over in range(chips):
            if up or over:
                signal_to(
                    barrier,
                    lax.rem(stage + up, stages),
                    lax.rem(z + over, chips) * 2 + core,
                )
    signal_to(barrier, stage, partner)
    pl.semaphore_wait(barrier, stages * chips)

    def farthest_first(send):
        for far in range(chips - 1, 0, -1):

            @pl.when(z + far < chips)
            def _():
                send(z + far)

            @pl.when(z - far >= 0)
            def _():
                send(z - far)

    def to_first(target):
        return pltpu.make_async_remote_copy(
            src_ref=x_ref,
            dst_ref=buf.at[stage, core, z],
            send_sem=in_send.at[target],
            recv_sem=direct_sem.at[stage],
            device_id={"pp": 0, "tp": target * 2 + core},
            device_id_type=pl.DeviceIdType.MESH,
        )

    farthest_first(lambda target: to_first(target).start())

    @pl.when(stage != 0)
    def _():
        to_first(z).start()

    @pl.when(stage == 0)
    def _():
        pltpu.make_async_copy(x_ref, buf.at[stage, core, z], direct_sem.at[stage]).start()

    head_of_lane = lax.broadcasted_iota(jnp.int32, (rows, cols), 1) // HEAD
    for part in range(2):
        piece = spike_ref[0, :, part * rows : (part + 1) * rows].T
        wide = jnp.zeros((rows, cols), F32)
        for h in range(heads):
            wide = jnp.where(head_of_lane == h, piece[:, h : h + 1], wide)
        spikes[part] = wide

    tri_row = lax.broadcasted_iota(jnp.int32, (rows, rows), 0)
    tri_col = lax.broadcasted_iota(jnp.int32, (rows, rows), 1)
    tril = tri_row >= tri_col
    tril_ones = jnp.where(tril, 1.0, 0.0).astype(BF16)
    tall_row = lax.rem(lax.broadcasted_iota(jnp.int32, (heads * rows, rows), 0), rows)
    tall_col = lax.broadcasted_iota(jnp.int32, (heads * rows, rows), 1)
    tall_mask = tall_row >= tall_col
    sq_row = lax.broadcasted_iota(jnp.int32, (cols, cols), 0) // HEAD
    sq_col = lax.broadcasted_iota(jnp.int32, (cols, cols), 1) // HEAD
    same_head = sq_row == sq_col
    mean_ones = jnp.where(same_head, 1.0 / HEAD, 0.0).astype(BF16)
    keep_span = 1.0 - low_ref[...]
    out_gain = jnp.concatenate([scale_ref[...]] * heads, axis=1)

    for load in loads:
        load.wait()

    def whole_wait(c, which, sem):
        half = buf.at[c, which]
        pltpu.make_async_copy(half, half, sem).wait()

    def forward(c):
        half = buf.at[c, core]
        return pltpu.make_async_remote_copy(
            src_ref=half,
            dst_ref=half,
            send_sem=forward_send.at[c],
            recv_sem=forward_sem.at[c],
            device_id={"pp": stage, "tp": partner},
            device_id_type=pl.DeviceIdType.MESH,
        )

    def to_next(c, target):
        return pltpu.make_async_remote_copy(
            src_ref=res.at[c],
            dst_ref=buf.at[c, core, z],
            send_sem=send_sem.at[c],
            recv_sem=direct_sem.at[c],
            device_id={"pp": lax.rem(stage + 1, stages), "tp": target * 2 + core},
            device_id_type=pl.DeviceIdType.MESH,
        )

    def to_out(c):
        return pltpu.make_async_remote_copy(
            src_ref=res.at[c],
            dst_ref=out_ref,
            send_sem=send_sem.at[c],
            recv_sem=out_sem,
            device_id={"pp": c, "tp": lane},
            device_id_type=pl.DeviceIdType.MESH,
        )

    def half_product(c, which):
        spans = [
            pl.ds(pl.multiple_of((2 * k + which) * cols, cols), cols) for k in range(chips)
        ]
        current = jnp.concatenate([buf[c, which, k] for k in range(chips)], axis=1).astype(F32)
        gain = jnp.concatenate([gain_ref[:, span] for span in spans], axis=1)
        matrix = jnp.concatenate([weights[:, span] for span in spans], axis=1)
        product = mm((current * gain).astype(BF16), matrix, NT)
        return product, jnp.sum(current * current, axis=1, keepdims=True)

    def step(c, carry):
        whole_wait(c, core, direct_sem.at[c])
        forward(c).start()

        if cols % 128 == 0:
            first, first_sum = half_product(c, core)
            whole_wait(c, 1 - core, forward_sem.at[c])
            second, second_sum = half_product(c, 1 - core)
            product, squares = first + second, first_sum + second_sum
        else:
            whole_wait(c, 1 - core, forward_sem.at[c])
            current = jnp.concatenate(
                [buf[c, k % 2, k // 2] for k in range(lanes_axis)], axis=1
            ).astype(F32)
            squares = jnp.sum(current * current, axis=1, keepdims=True)
            scaled = (current * gain_ref[...]).astype(BF16)
            product = mm(scaled, weights[...], NT)
        projected = product * lax.rsqrt(squares / width + EPSILON)
        query_pre = projected[:, 0 * cols : 1 * cols]
        forget_pre = projected[:, 1 * cols : 2 * cols]
        values = projected[:, 2 * cols : 3 * cols].astype(BF16)
        gate_pre = projected[:, 3 * cols : 4 * cols]

        key_in = keep_span * sigmoid(-forget_pre)
        log_forget = jnp.log(1.0 - key_in) + spikes[lax.rem(c, 2)]
        high = log_forget.astype(BF16)
        low = (log_forget - high.astype(F32)).astype(BF16)
        running = mm(tril_ones, high, NN) + mm(tril_ones, low, NN)
        ending = running[rows - 1 : rows, :]
        query_scaled = query_pre * sigmoid(query_pre) * jnp.exp(running)
        key_scaled = (key_in * jnp.exp(-running)).astype(BF16)
        key_end = (key_in * jnp.exp(ending - running)).astype(BF16)
        query_bf = query_scaled.astype(BF16)
        tall_query = jnp.concatenate(
            [jnp.where(head_of_lane == h, query_scaled, 0.0).astype(BF16) for h in range(heads)],
            axis=0,
        )
        scores = jnp.where(tall_mask, mm(tall_query, key_scaled, NT), 0.0).astype(BF16)
        tall_mixed = mm(scores, values, NN)
        memory = jnp.where(lax.rem(c, 2) == 0, 0.0, state[...])
        mixed = mm(query_bf, memory.astype(BF16), NT)
        inner = tall_mixed[0:rows]
        for h in range(1, heads):
            inner = jnp.where(head_of_lane == h, tall_mixed[h * rows : (h + 1) * rows], inner)
        mixed = mixed + inner
        mean_square = mm((mixed * mixed).astype(BF16), mean_ones, NN)
        branch = mixed * lax.rsqrt(mean_square + EPSILON) * out_gain
        branch = branch * (gate_pre * sigmoid(gate_pre))
        res[c] = (buf[c, core, z].astype(F32) + branch).astype(BF16)

        @pl.when(stage != stages - 1)
        def _():
            farthest_first(lambda target: to_next(c, target).start())
            to_next(c, z).start()

        @pl.when((stage == stages - 1) & (c != stage))
        def _():
            to_out(c).start()

        @pl.when((stage == stages - 1) & (c == stage))
        def _():
            pltpu.make_async_copy(res.at[c], out_ref, out_sem).start()

        added = jnp.where(same_head, mm(values, key_end, TN), 0.0)
        state[...] = memory * jnp.exp(ending) + added
        return carry

    lax.fori_loop(0, chunks, step, 0)

    farthest_first(lambda target: to_first(target).wait_send())

    @pl.when(stage != 0)
    def _():
        to_first(z).wait_send()

    def drain(c, carry):
        forward(c).wait_send()

        @pl.when(stage != stages - 1)
        def _():
            whole_wait(c, core, send_sem.at[c])

        @pl.when((stage == stages - 1) & (c != stage))
        def _():
            to_out(c).wait_send()

        return carry

    lax.fori_loop(0, chunks, drain, 0)
    pltpu.make_async_copy(out_ref, out_ref, out_sem).wait()


def solution(mesh):
    stages = mesh.shape["pp"]
    lanes_axis = mesh.shape["tp"]
    chips = lanes_axis // 2

    def step(x, gain, wq, wf, wi, wg, low, spike, scale):
        rows, cols = x.shape
        width = gain.shape[1]
        vmem = pl.BlockSpec(memory_space=pltpu.VMEM)
        hbm = pl.BlockSpec(memory_space=pl.ANY)
        dma = pltpu.SemaphoreType.DMA
        return pl.pallas_call(
            functools.partial(kernel, stages, lanes_axis),
            out_shape=jax.ShapeDtypeStruct((rows, cols), BF16),
            in_specs=[vmem, vmem, hbm, hbm, hbm, hbm, vmem, vmem, vmem],
            out_specs=vmem,
            scratch_shapes=[
                pltpu.VMEM((4 * cols, width), BF16),
                pltpu.VMEM((stages, 2, chips, rows, cols), BF16),
                pltpu.VMEM((stages, rows, cols), BF16),
                pltpu.VMEM((2, rows, cols), F32),
                pltpu.VMEM((cols, cols), F32),
                dma((4,)),
                dma((chips,)),
                dma((stages,)),
                dma((stages,)),
                dma((stages,)),
                dma((stages,)),
                dma,
            ],
            compiler_params=pltpu.CompilerParams(
                collective_id=0, has_side_effects=True, vmem_limit_bytes=67043328
            ),
        )(x, gain, wq, wf, wi, wg, low, spike.transpose(0, 2, 1), scale)

    in_specs = (
        P("pp", "tp"),
        P("pp", None),
        P("pp", "tp", None),
        P("pp", "tp", None),
        P("pp", "tp", None),
        P("pp", "tp", None),
        P("pp", "tp"),
        P("pp", None, "tp"),
        P("pp", None),
    )
    return jax.shard_map(
        step, mesh=mesh, in_specs=in_specs, out_specs=P("pp", "tp"), check_vma=False
    )
```

```python
import functools

import jax
import jax.numpy as jnp
from jax import lax
from jax.experimental import pallas as pl
from jax.experimental.pallas import tpu as pltpu
from jax.sharding import PartitionSpec as P

HEAD = 64
TILE = 256
EPSILON = 1e-06
F32 = jnp.float32
BF16 = jnp.bfloat16
NT = (((1,), (1,)), ((), ()))
NN = (((1,), (0,)), ((), ()))
TN = (((0,), (0,)), ((), ()))


def mm(a, b, dims):
    return lax.dot_general(a, b, dims, preferred_element_type=F32)


def sigmoid(v):
    return 1.0 / (1.0 + jnp.exp(-v))


def signal_to(semaphore, stage, lane):
    pl.semaphore_signal(
        semaphore,
        inc=1,
        device_id={"pp": stage, "tp": lane},
        device_id_type=pl.DeviceIdType.MESH,
    )


def kernel(
    stages,
    lanes_axis,
    x_ref,
    gain_ref,
    wq_ref,
    wf_ref,
    wi_ref,
    wg_ref,
    low_ref,
    spike_ref,
    scale_ref,
    out_ref,
    weights,
    turned,
    buf,
    res,
    spikes,
    state,
    w_sem,
    in_send,
    direct_sem,
    forward_sem,
    send_sem,
    forward_send,
    out_sem,
):
    rows, cols = x_ref.shape
    heads = cols // HEAD
    width = gain_ref.shape[1]
    chips = lanes_axis // 2
    chunks = stages
    stage = lax.axis_index("pp")
    lane = lax.axis_index("tp")
    core = lax.rem(lane, 2)
    z = lane // 2
    partner = z * 2 + (1 - core)

    loads = []
    for role, ref in enumerate((wq_ref, wf_ref, wi_ref, wg_ref)):
        load = pltpu.make_async_copy(
            ref.at[0], weights.at[pl.ds(role * cols, cols)], w_sem.at[role]
        )
        load.start()
        loads.append(load)

    barrier = pltpu.get_barrier_semaphore()
    for up in range(stages):
        for over in range(chips):
            if up or over:
                signal_to(
                    barrier,
                    lax.rem(stage + up, stages),
                    lax.rem(z + over, chips) * 2 + core,
                )
    signal_to(barrier, stage, partner)
    pl.semaphore_wait(barrier, stages * chips)

    def farthest_first(send):
        for far in range(chips - 1, 0, -1):

            @pl.when(z + far < chips)
            def _():
                send(z + far)

            @pl.when(z - far >= 0)
            def _():
                send(z - far)

    def to_first(target):
        return pltpu.make_async_remote_copy(
            src_ref=x_ref,
            dst_ref=buf.at[stage, core, z],
            send_sem=in_send.at[target],
            recv_sem=direct_sem.at[stage],
            device_id={"pp": 0, "tp": target * 2 + core},
            device_id_type=pl.DeviceIdType.MESH,
        )

    farthest_first(lambda target: to_first(target).start())

    @pl.when(stage != 0)
    def _():
        to_first(z).start()

    @pl.when(stage == 0)
    def _():
        pltpu.make_async_copy(x_ref, buf.at[stage, core, z], direct_sem.at[stage]).start()

    head_of_lane = lax.broadcasted_iota(jnp.int32, (rows, cols), 1) // HEAD
    for part in range(2):
        piece = spike_ref[0, :, part * rows : (part + 1) * rows].T
        wide = jnp.zeros((rows, cols), F32)
        for h in range(heads):
            wide = jnp.where(head_of_lane == h, piece[:, h : h + 1], wide)
        spikes[part] = wide

    tri_row = lax.broadcasted_iota(jnp.int32, (rows, rows), 0)
    tri_col = lax.broadcasted_iota(jnp.int32, (rows, rows), 1)
    tril = tri_row >= tri_col
    tril_ones = jnp.where(tril, 1.0, 0.0).astype(BF16)
    tall_row = lax.rem(lax.broadcasted_iota(jnp.int32, (heads * rows, rows), 0), rows)
    tall_col = lax.broadcasted_iota(jnp.int32, (heads * rows, rows), 1)
    tall_mask = tall_row >= tall_col
    sq_row = lax.broadcasted_iota(jnp.int32, (cols, cols), 0) // HEAD
    sq_col = lax.broadcasted_iota(jnp.int32, (cols, cols), 1) // HEAD
    same_head = sq_row == sq_col
    mean_ones = jnp.where(same_head, 1.0 / HEAD, 0.0).astype(BF16)
    keep_span = 1.0 - low_ref[...]
    out_gain = jnp.concatenate([scale_ref[...]] * heads, axis=1)

    for role, load in enumerate(loads):
        load.wait()

        def turn(k, carry, role=role):
            tile = pl.ds(pl.multiple_of(k * TILE, TILE), TILE)
            turned[tile, role * cols : (role + 1) * cols] = weights[
                role * cols : (role + 1) * cols, tile
            ].T
            return carry

        lax.fori_loop(0, width // TILE, turn, 0)

    def whole_wait(c, which, sem):
        half = buf.at[c, which]
        pltpu.make_async_copy(half, half, sem).wait()

    def forward(c):
        half = buf.at[c, core]
        return pltpu.make_async_remote_copy(
            src_ref=half,
            dst_ref=half,
            send_sem=forward_send.at[c],
            recv_sem=forward_sem.at[c],
            device_id={"pp": stage, "tp": partner},
            device_id_type=pl.DeviceIdType.MESH,
        )

    def to_next(c, target):
        return pltpu.make_async_remote_copy(
            src_ref=res.at[c],
            dst_ref=buf.at[c, core, z],
            send_sem=send_sem.at[c],
            recv_sem=direct_sem.at[c],
            device_id={"pp": lax.rem(stage + 1, stages), "tp": target * 2 + core},
            device_id_type=pl.DeviceIdType.MESH,
        )

    def to_out(c):
        return pltpu.make_async_remote_copy(
            src_ref=res.at[c],
            dst_ref=out_ref,
            send_sem=send_sem.at[c],
            recv_sem=out_sem,
            device_id={"pp": c, "tp": lane},
            device_id_type=pl.DeviceIdType.MESH,
        )

    def step(c, carry):
        whole_wait(c, core, direct_sem.at[c])
        forward(c).start()

        whole_wait(c, 1 - core, forward_sem.at[c])
        current = jnp.concatenate(
            [buf[c, k % 2, k // 2] for k in range(lanes_axis)], axis=1
        ).astype(F32)
        squares = jnp.sum(current * current, axis=1, keepdims=True)
        scaled = (current * gain_ref[...]).astype(BF16)
        product = mm(scaled, turned[...], NN)
        projected = product * lax.rsqrt(squares / width + EPSILON)
        query_pre = projected[:, 0 * cols : 1 * cols]
        forget_pre = projected[:, 1 * cols : 2 * cols]
        values = projected[:, 2 * cols : 3 * cols].astype(BF16)
        gate_pre = projected[:, 3 * cols : 4 * cols]

        key_in = keep_span * sigmoid(-forget_pre)
        log_forget = jnp.log(1.0 - key_in) + spikes[lax.rem(c, 2)]
        high = log_forget.astype(BF16)
        low = (log_forget - high.astype(F32)).astype(BF16)
        running = mm(tril_ones, high, NN) + mm(tril_ones, low, NN)
        ending = running[rows - 1 : rows, :]
        query_scaled = query_pre * sigmoid(query_pre) * jnp.exp(running)
        key_scaled = (key_in * jnp.exp(-running)).astype(BF16)
        key_end = (key_in * jnp.exp(ending - running)).astype(BF16)
        query_bf = query_scaled.astype(BF16)
        tall_query = jnp.concatenate(
            [jnp.where(head_of_lane == h, query_scaled, 0.0).astype(BF16) for h in range(heads)],
            axis=0,
        )
        scores = jnp.where(tall_mask, mm(tall_query, key_scaled, NT), 0.0).astype(BF16)
        tall_mixed = mm(scores, values, NN)
        memory = jnp.where(lax.rem(c, 2) == 0, 0.0, state[...])
        mixed = mm(query_bf, memory.astype(BF16), NT)
        inner = tall_mixed[0:rows]
        for h in range(1, heads):
            inner = jnp.where(head_of_lane == h, tall_mixed[h * rows : (h + 1) * rows], inner)
        mixed = mixed + inner
        mean_square = mm((mixed * mixed).astype(BF16), mean_ones, NN)
        branch = mixed * lax.rsqrt(mean_square + EPSILON) * out_gain
        branch = branch * (gate_pre * sigmoid(gate_pre))
        res[c] = (buf[c, core, z].astype(F32) + branch).astype(BF16)

        @pl.when(stage != stages - 1)
        def _():
            farthest_first(lambda target: to_next(c, target).start())
            to_next(c, z).start()

        @pl.when((stage == stages - 1) & (c != stage))
        def _():
            to_out(c).start()

        @pl.when((stage == stages - 1) & (c == stage))
        def _():
            pltpu.make_async_copy(res.at[c], out_ref, out_sem).start()

        added = jnp.where(same_head, mm(values, key_end, TN), 0.0)
        state[...] = memory * jnp.exp(ending) + added
        return carry

    lax.fori_loop(0, chunks, step, 0)

    farthest_first(lambda target: to_first(target).wait_send())

    @pl.when(stage != 0)
    def _():
        to_first(z).wait_send()

    def drain(c, carry):
        forward(c).wait_send()

        @pl.when(stage != stages - 1)
        def _():
            whole_wait(c, core, send_sem.at[c])

        @pl.when((stage == stages - 1) & (c != stage))
        def _():
            to_out(c).wait_send()

        return carry

    lax.fori_loop(0, chunks, drain, 0)
    pltpu.make_async_copy(out_ref, out_ref, out_sem).wait()


def solution(mesh):
    stages = mesh.shape["pp"]
    lanes_axis = mesh.shape["tp"]
    chips = lanes_axis // 2

    def step(x, gain, wq, wf, wi, wg, low, spike, scale):
        rows, cols = x.shape
        width = gain.shape[1]
        vmem = pl.BlockSpec(memory_space=pltpu.VMEM)
        hbm = pl.BlockSpec(memory_space=pl.ANY)
        dma = pltpu.SemaphoreType.DMA
        return pl.pallas_call(
            functools.partial(kernel, stages, lanes_axis),
            out_shape=jax.ShapeDtypeStruct((rows, cols), BF16),
            in_specs=[vmem, vmem, hbm, hbm, hbm, hbm, vmem, vmem, vmem],
            out_specs=vmem,
            scratch_shapes=[
                pltpu.VMEM((4 * cols, width), BF16),
                pltpu.VMEM((width, 4 * cols), BF16),
                pltpu.VMEM((stages, 2, chips, rows, cols), BF16),
                pltpu.VMEM((stages, rows, cols), BF16),
                pltpu.VMEM((2, rows, cols), F32),
                pltpu.VMEM((cols, cols), F32),
                dma((4,)),
                dma((chips,)),
                dma((stages,)),
                dma((stages,)),
                dma((stages,)),
                dma((stages,)),
                dma,
            ],
            compiler_params=pltpu.CompilerParams(
                collective_id=0, has_side_effects=True, vmem_limit_bytes=67043328
            ),
        )(x, gain, wq, wf, wi, wg, low, spike.transpose(0, 2, 1), scale)

    in_specs = (
        P("pp", "tp"),
        P("pp", None),
        P("pp", "tp", None),
        P("pp", "tp", None),
        P("pp", "tp", None),
        P("pp", "tp", None),
        P("pp", "tp"),
        P("pp", None, "tp"),
        P("pp", None),
    )
    return jax.shard_map(
        step, mesh=mesh, in_specs=in_specs, out_specs=P("pp", "tp"), check_vma=False
    )
```
